32 devices in a mesh: sp: 8 (over z, x), tp: 4 (over y, core).
Axes of the slice: x: 2, y: 2, z: 4, core: 2. Of those that a mesh axis runs over, the one named last changes fastest.
Arguments:
- residual: bfloat16 [4096, 4096], P('sp'), may hold values from -6 to 6
- queries: bfloat16 [4096, 1024], P('sp', 'tp'), may hold values from -6 to 6
- projected_key_rows: bfloat16 [4096, 1024], P('sp', 'tp'), may hold values from -6 to 6
- projected_value_rows: bfloat16 [4096, 2048], P('sp', 'tp'), may hold values from -6 to 6
- output_gate_logits: bfloat16 [4096, 2048], P('sp', 'tp'), may hold values from -6 to 6
- input_gate_logits: float32 [16, 4096], P('tp', 'sp'), may hold values from -8 to 120
- forget_gate_logits: float32 [16, 4096], P('tp', 'sp'), may hold values from 0 to 16
- extra_forget_logits: float32 [16, 4096], P('tp', 'sp'), may hold values from -0.7 to 0, as said below
- head_norm_gain: bfloat16 [2048], P('tp'), may hold values from 0.099609375 to 1.8984375
- output_projection_weight: bfloat16 [2048, 4096], P('tp'), may hold values from -0.125 to 0.125
- feedforward_norm_gain: bfloat16 [4096], replicated, may hold values from 0.099609375 to 1.8984375
- feedforward_gate_weight: bfloat16 [4096, 11264], P('sp', 'tp'), may hold values from -0.09375 to 0.09375
- up_projection_weight: bfloat16 [4096, 11264], P('sp', 'tp'), may hold values from -0.09375 to 0.09375
- down_projection_weight: bfloat16 [4096, 11264], P('sp', 'tp'), may hold values from -0.0546875 to 0.0546875
Outputs:
- layer_out: bfloat16 [4096, 4096], P(('sp', 'tp'))
The draws below stay inside these ranges and needn't reach their ends.
Inputs may be any that keep to these rules, and one draw needn't show every extreme that they name: `extra_forget_logits`: each entry is 0 or the logarithm of a factor between one half and 0.8.
All inputs are finite; a program needn't handle non-finite values.
Results may differ from the reference program's by a relative error of at most 0.01.
Values may be sent and summed in bfloat16 or wider, within the bound.
A program may use at most 192 MiB of HBM per device.

```python
import math
import jax
import jax.numpy as jnp
from jax import lax

D = 4096
HEADS = 16
QK_DIM = 64
V_DIM = 128
FF = 11264
BLOCK = 64
TOK_DEV = 512
TOKENS = 4096
VW = 2048
N_TP = 4


def draw_input_gate_logits(key, part):
    values = jnp.clip(1.5 * jax.random.normal(jax.random.fold_in(key, 11), (HEADS, TOKENS), jnp.float32), -6.0, 6.0)
    return values.astype(jnp.float32)


def draw_forget_gate_logits(key, part):
    slow = jax.random.bernoulli(jax.random.fold_in(key, 21), 0.5, (HEADS, 1))
    noise = 0.7 * jax.random.normal(jax.random.fold_in(key, 22), (HEADS, TOKENS), jnp.float32)
    base = jnp.where(slow, math.log(TOKENS) + 1.5, 3.5)
    shift = jax.random.uniform(jax.random.fold_in(key, 23), (HEADS, TOKENS // TOK_DEV), jnp.float32, -0.7, 0.7)
    values = base + noise + jnp.repeat(shift, TOK_DEV, axis=1)
    return jnp.clip(values, 0.0, 16.0).astype(jnp.float32)


def draw_extra_forget_logits(key, part):
    hits = jax.random.bernoulli(jax.random.fold_in(key, 31), 4.0 / TOKENS, (HEADS, TOKENS))
    factor = jax.random.uniform(jax.random.fold_in(key, 32), (HEADS, TOKENS), jnp.float32, 0.5, 0.8)
    return jnp.where(hits, jnp.log(factor), 0.0).astype(jnp.float32)


def block_levels(rng, shape, split, least, top_value):
    def one(dim, parts):
        draws = jax.random.uniform(jax.random.fold_in(jax.random.fold_in(rng, 6), dim), (parts,), jnp.float32, least / len(split), top_value / len(split))
        return jnp.repeat(jnp.exp(draws), shape[dim] // parts).reshape((-1,) + (1,) * (len(shape) - dim - 1))

    level = one(*split[0])
    for cut in split[1:]:
        level = level * one(*cut)
    return level


def centred(key, extent, scale, bound, cuts=(), kind=jnp.bfloat16):
    drawn = scale * jax.random.normal(key, extent, jnp.float32)
    if cuts:
        drawn = drawn * block_levels(key, extent, cuts, -0.22, 0.18)
    return jnp.clip(drawn, -bound, bound).astype(kind)


def setup_inputs(seed: int = 0) -> dict:
    streams_of = jax.random.split(jax.random.key(seed), 15)
    residual = centred(streams_of[0], (TOKENS, D), 1.0, 6.0, ((0, 8),))
    queries = centred(streams_of[1], (TOKENS, HEADS * QK_DIM), 1.0, 6.0, ((0, 8), (1, 4)))
    projected_key_rows = centred(streams_of[2], (TOKENS, HEADS * QK_DIM), 1.0, 6.0, ((0, 8), (1, 4)))
    projected_value_rows = centred(streams_of[3], (TOKENS, VW), 1.0, 6.0, ((0, 8), (1, 4)))
    output_gate_logits = centred(streams_of[4], (TOKENS, VW), 1.0, 6.0, ((0, 8), (1, 4)))
    input_gate_logits = draw_input_gate_logits(jax.random.fold_in(streams_of[14], 71), 0)
    forget_gate_logits = draw_forget_gate_logits(jax.random.fold_in(streams_of[14], 71), 0)
    extra_forget_logits = draw_extra_forget_logits(jax.random.fold_in(streams_of[14], 71), 0)
    head_norm_gain = jnp.clip(1.0 + 0.18 * jax.random.normal(streams_of[8], (VW,), jnp.float32), 0.099609375, 1.8984375).astype(jnp.bfloat16)
    output_projection_weight = centred(streams_of[9], (VW, D), VW ** -0.5, 0.125, ((0, 4),))
    feedforward_norm_gain = jnp.clip(1.0 + 0.18 * jax.random.normal(streams_of[10], (D,), jnp.float32), 0.099609375, 1.8984375).astype(jnp.bfloat16)
    feedforward_gate_weight = centred(streams_of[11], (D, FF), D ** -0.5, 0.09375, ((0, 8), (1, 4)))
    up_projection_weight = centred(streams_of[12], (D, FF), D ** -0.5, 0.09375, ((0, 8), (1, 4)))
    down_projection_weight = centred(streams_of[13], (D, FF), FF ** -0.5, 0.0546875, ((0, 8), (1, 4)))
    return {"residual": residual, "queries": queries, "projected_key_rows": projected_key_rows, "projected_value_rows": projected_value_rows, "output_gate_logits": output_gate_logits, "input_gate_logits": input_gate_logits, "forget_gate_logits": forget_gate_logits, "extra_forget_logits": extra_forget_logits, "head_norm_gain": head_norm_gain, "output_projection_weight": output_projection_weight, "feedforward_norm_gain": feedforward_norm_gain, "feedforward_gate_weight": feedforward_gate_weight, "up_projection_weight": up_projection_weight, "down_projection_weight": down_projection_weight}


def run_blocks(query_h, key_h, value_h, gate_in, forget_logarithm, state_init, norm_init, peak_init):
    span_len = BLOCK
    blocks_count = query_h.shape[0] // span_len
    query_b = query_h.reshape(blocks_count, span_len, query_h.shape[1])
    key_b = key_h.reshape(blocks_count, span_len, key_h.shape[1])
    value_b = value_h.reshape(blocks_count, span_len, value_h.shape[1])
    gate_b = gate_in.reshape(blocks_count, span_len)
    cum_local = jnp.cumsum(forget_logarithm.reshape(blocks_count, span_len), axis=1)
    cum_last = cum_local[:, -1]
    log_end = cum_last[:, None] - cum_local + gate_b

    def advance(carry, inputs):
        state_now, norm_now, peak_now = carry
        key_blk, value_blk, log_blk, last_blk = inputs
        peak_next = jnp.maximum(last_blk + peak_now, jnp.max(log_blk))
        decay_now = jnp.exp(last_blk + peak_now - peak_next)
        weights = jnp.exp(log_blk - peak_next)
        state_next = decay_now * state_now + jnp.einsum('l,lv,lk->vk', weights, value_blk, key_blk, precision=lax.Precision.HIGHEST)
        norm_next = decay_now * norm_now + jnp.einsum('l,lk->k', weights, key_blk, precision=lax.Precision.HIGHEST)
        return ((state_next, norm_next, peak_next), (state_now, norm_now, peak_now))
    carried, (state_prev, norm_prev, peak_prev) = lax.scan(advance, (state_init, norm_init, peak_init), (key_b, value_b, log_end, cum_last))
    causal = jnp.tril(jnp.ones((span_len, span_len), dtype=bool))
    log_pair = cum_local[:, :, None] - cum_local[:, None, :] + gate_b[:, None, :]
    log_pair = jnp.where(causal[None], log_pair, -jnp.inf)
    inter_log = cum_local + peak_prev[:, None]
    peak_row = jnp.maximum(inter_log, lax.optimization_barrier(jnp.max(log_pair, axis=2)))
    scores = jnp.einsum('cjk,csk->cjs', query_b, key_b, precision=lax.Precision.HIGHEST) * jnp.exp(log_pair - peak_row[:, :, None])
    inter_scale = jnp.exp(inter_log - peak_row)
    numer = jnp.einsum('cjs,csv->cjv', scores, value_b, precision=lax.Precision.HIGHEST)
    numer = numer + inter_scale[:, :, None] * jnp.einsum('cjk,cvk->cjv', query_b, state_prev, precision=lax.Precision.HIGHEST)
    denominator = lax.optimization_barrier(jnp.sum(scores, axis=2)) + inter_scale * jnp.einsum('cjk,ck->cj', query_b, norm_prev, precision=lax.Precision.HIGHEST)
    cell_out = numer / jnp.maximum(jnp.abs(denominator), jnp.exp(-peak_row))[:, :, None]
    return cell_out.reshape(query_h.shape[0], value_h.shape[1])

def by_heads(rows, heads_count):
    tok_count = rows.shape[0]
    return rows.astype(jnp.float32).reshape(tok_count, heads_count, rows.shape[1] // heads_count).transpose(1, 0, 2)

def rms_scaled(values_f32, gain):
    mean_square = lax.optimization_barrier(jnp.mean(values_f32 * values_f32, axis=-1, keepdims=True))
    return values_f32 * lax.rsqrt(mean_square + 1e-06) * gain.astype(jnp.float32)

def reference(residual, queries, projected_key_rows, projected_value_rows, output_gate_logits, input_gate_logits, forget_gate_logits, extra_forget_logits, head_norm_gain, output_projection_weight, feedforward_norm_gain, feedforward_gate_weight, up_projection_weight, down_projection_weight):
    query_h = by_heads(queries, HEADS) * QK_DIM ** (-0.5)
    key_h = by_heads(projected_key_rows, HEADS)
    value_h = by_heads(projected_value_rows, HEADS)
    forget_logarithm = jax.nn.log_sigmoid(forget_gate_logits) + extra_forget_logits
    state_zero = jnp.zeros((HEADS, V_DIM, QK_DIM), jnp.float32)
    norm_zero = jnp.zeros((HEADS, QK_DIM), jnp.float32)
    peak_zero = jnp.zeros((HEADS,), jnp.float32)
    cell_out = jax.vmap(run_blocks)(query_h, key_h, value_h, input_gate_logits, forget_logarithm, state_zero, norm_zero, peak_zero)
    normed_heads = rms_scaled(cell_out, head_norm_gain.reshape(HEADS, 1, V_DIM))
    gated = (normed_heads.transpose(1, 0, 2).reshape(TOKENS, VW) * jax.nn.sigmoid(output_gate_logits.astype(jnp.float32))).astype(jnp.bfloat16)
    group_cols = VW // N_TP
    attn_sum = jnp.zeros((TOKENS, D), jnp.float32)
    for group in range(N_TP):
        partial_out = jnp.dot(gated[:, group * group_cols:(group + 1) * group_cols], output_projection_weight[group * group_cols:(group + 1) * group_cols], preferred_element_type=jnp.float32).astype(jnp.bfloat16)
        attn_sum = attn_sum + lax.optimization_barrier(partial_out).astype(jnp.float32)
    stream = residual.astype(jnp.float32) + attn_sum
    normed = rms_scaled(stream, feedforward_norm_gain).astype(jnp.bfloat16)
    gate_pre = jnp.dot(normed, feedforward_gate_weight, preferred_element_type=jnp.float32)
    up_pre = jnp.dot(normed, up_projection_weight, preferred_element_type=jnp.float32)
    hidden = (jax.nn.silu(gate_pre) * up_pre).astype(jnp.bfloat16)
    hidden_cols = FF // N_TP
    ffn_sum = jnp.zeros((TOKENS, D), jnp.float32)
    for group in range(N_TP):
        partial_ffn = lax.dot_general(hidden[:, group * hidden_cols:(group + 1) * hidden_cols], down_projection_weight[:, group * hidden_cols:(group + 1) * hidden_cols], (((1,), (1,)), ((), ())), preferred_element_type=jnp.float32).astype(jnp.bfloat16)
        ffn_sum = ffn_sum + lax.optimization_barrier(partial_ffn).astype(jnp.float32)
    return (stream + 0.5 * ffn_sum).astype(jnp.bfloat16)
```

```python
import jax
import jax.numpy as jnp
from jax import lax
from jax.sharding import PartitionSpec as P

QK_DIM = 64
V_DIM = 128
BLOCK = 64


def entering(part, axis, combine, identity):
    place = lax.axis_index(axis)
    gathered = jax.tree.map(lambda a: lax.all_gather(a, axis), part)
    state = jax.tree.map(lambda a, e: jnp.zeros_like(a) + jnp.asarray(e, a.dtype), part, identity)

    def one(step, state):
        return combine(
            state, jax.tree.map(lambda a: lax.dynamic_index_in_dim(a, step, 0, False), gathered)
        )

    return lax.fori_loop(0, place, one, state)


def run_blocks(
    query_h, key_h, value_h, gate_in, forget_logarithm, state_init, norm_init, peak_init
):
    span_len = BLOCK
    blocks_count = query_h.shape[0] // span_len
    query_b = query_h.reshape(blocks_count, span_len, query_h.shape[1])
    key_b = key_h.reshape(blocks_count, span_len, key_h.shape[1])
    value_b = value_h.reshape(blocks_count, span_len, value_h.shape[1])
    gate_b = gate_in.reshape(blocks_count, span_len)
    cum_local = jnp.cumsum(forget_logarithm.reshape(blocks_count, span_len), axis=1)
    cum_last = cum_local[:, -1]
    log_end = cum_last[:, None] - cum_local + gate_b

    def advance(carry, inputs):
        state_now, norm_now, peak_now = carry
        key_blk, value_blk, log_blk, last_blk = inputs
        peak_next = jnp.maximum(last_blk + peak_now, jnp.max(log_blk))
        decay_now = jnp.exp(last_blk + peak_now - peak_next)
        weights = jnp.exp(log_blk - peak_next)
        state_next = decay_now * state_now + jnp.einsum(
            "l,lv,lk->vk", weights, value_blk, key_blk, precision=lax.Precision.HIGHEST
        )
        norm_next = decay_now * norm_now + jnp.einsum(
            "l,lk->k", weights, key_blk, precision=lax.Precision.HIGHEST
        )
        return ((state_next, norm_next, peak_next), (state_now, norm_now, peak_now))

    carried, (state_prev, norm_prev, peak_prev) = lax.scan(
        advance, (state_init, norm_init, peak_init), (key_b, value_b, log_end, cum_last)
    )
    causal = jnp.tril(jnp.ones((span_len, span_len), dtype=bool))
    log_pair = cum_local[:, :, None] - cum_local[:, None, :] + gate_b[:, None, :]
    log_pair = jnp.where(causal[None], log_pair, -jnp.inf)
    inter_log = cum_local + peak_prev[:, None]
    peak_row = jnp.maximum(inter_log, jnp.max(log_pair, axis=2))
    scores = jnp.einsum("cjk,csk->cjs", query_b, key_b, precision=lax.Precision.HIGHEST) * jnp.exp(
        log_pair - peak_row[:, :, None]
    )
    inter_scale = jnp.exp(inter_log - peak_row)
    numer = jnp.einsum("cjs,csv->cjv", scores, value_b, precision=lax.Precision.HIGHEST)
    numer = numer + inter_scale[:, :, None] * jnp.einsum(
        "cjk,cvk->cjv", query_b, state_prev, precision=lax.Precision.HIGHEST
    )
    denominator = jnp.sum(scores, axis=2) + inter_scale * jnp.einsum(
        "cjk,ck->cj", query_b, norm_prev, precision=lax.Precision.HIGHEST
    )
    cell_out = numer / jnp.maximum(jnp.abs(denominator), jnp.exp(-peak_row))[:, :, None]
    return cell_out.reshape(query_h.shape[0], value_h.shape[1])


def by_heads(rows, heads_count):
    tok_count = rows.shape[0]
    return (
        rows.astype(jnp.float32)
        .reshape(tok_count, heads_count, rows.shape[1] // heads_count)
        .transpose(1, 0, 2)
    )


def rms_scaled(values_f32, gain):
    mean_square = jnp.mean(values_f32 * values_f32, axis=-1, keepdims=True)
    return values_f32 * lax.rsqrt(mean_square + 1e-06) * gain.astype(jnp.float32)


def joined(earlier, later):
    total_e, state_e, norm_e, peak_e = earlier
    total_l, state_l, norm_l, peak_l = later
    peak_both = jnp.maximum(total_l + peak_e, peak_l)
    weight_e = jnp.exp(total_l + peak_e - peak_both)
    weight_l = jnp.exp(peak_l - peak_both)
    state_both = weight_e[:, None, None] * state_e + weight_l[:, None, None] * state_l
    norm_both = weight_e[:, None] * norm_e + weight_l[:, None] * norm_l
    return (total_e + total_l, state_both, norm_both, peak_both)


def exchanged(gate, up, down, axis):
    parts = lax.axis_size(axis)
    place = lax.axis_index(axis)
    rows, cols = gate.shape
    hid = cols // parts
    chunks = jnp.stack(
        [
            jnp.stack([w[:, p * hid : (p + 1) * hid] for w in (gate, up, down)])
            for p in range(parts)
        ]
    )
    whole = jnp.zeros_like(chunks)
    own = lax.dynamic_index_in_dim(chunks, place, 0, False)
    whole = lax.dynamic_update_index_in_dim(whole, own, place, 0)
    for shift in range(1, parts):
        sent = lax.dynamic_index_in_dim(chunks, lax.rem(place + shift, parts), 0, False)
        got = lax.ppermute(sent, axis, [(i, (i + shift) % parts) for i in range(parts)])
        whole = lax.dynamic_update_index_in_dim(
            whole, got, lax.rem(place - shift + parts, parts), 0
        )
    return whole


def per_device(
    residual,
    queries,
    projected_key_rows,
    projected_value_rows,
    output_gate_logits,
    input_gate_logits,
    forget_gate_logits,
    extra_forget_logits,
    head_norm_gain,
    output_projection_weight,
    feedforward_norm_gain,
    feedforward_gate_weight,
    up_projection_weight,
    down_projection_weight,
):
    weights = exchanged(
        feedforward_gate_weight, up_projection_weight, down_projection_weight, "sp"
    )
    tok_here = queries.shape[0]
    heads_here = input_gate_logits.shape[0]
    own_rows = tok_here // lax.axis_size("tp")
    query_h = by_heads(queries, heads_here) * QK_DIM ** (-0.5)
    key_h = by_heads(projected_key_rows, heads_here)
    value_h = by_heads(projected_value_rows, heads_here)
    forget_logarithm = jax.nn.log_sigmoid(forget_gate_logits) + extra_forget_logits
    cum_shard = jnp.cumsum(forget_logarithm, axis=1)
    total_shard = cum_shard[:, -1]
    log_shard = total_shard[:, None] - cum_shard + input_gate_logits
    peak_shard = jnp.max(log_shard, axis=1)
    weight_shard = jnp.exp(log_shard - peak_shard[:, None])
    state_shard = jnp.einsum(
        "hl,hlv,hlk->hvk", weight_shard, value_h, key_h, precision=lax.Precision.HIGHEST
    )
    norm_shard = jnp.einsum("hl,hlk->hk", weight_shard, key_h, precision=lax.Precision.HIGHEST)
    identity = (
        jnp.zeros((heads_here,), jnp.float32),
        jnp.zeros_like(state_shard),
        jnp.zeros_like(norm_shard),
        jnp.full((heads_here,), -1e30, jnp.float32),
    )
    total_before, state_before, norm_before, peak_before = entering(
        (total_shard, state_shard, norm_shard, peak_shard), "sp", joined, identity
    )
    peak_in = jnp.maximum(peak_before, total_before)
    rescale = jnp.exp(peak_before - peak_in)
    state_in = rescale[:, None, None] * state_before
    norm_in = rescale[:, None] * norm_before
    cell_out = jax.vmap(run_blocks)(
        query_h, key_h, value_h, input_gate_logits, forget_logarithm, state_in, norm_in, peak_in
    )
    normed_heads = rms_scaled(cell_out, head_norm_gain.reshape(heads_here, 1, V_DIM))
    gated = (
        normed_heads.transpose(1, 0, 2).reshape(tok_here, heads_here * V_DIM)
        * jax.nn.sigmoid(output_gate_logits.astype(jnp.float32))
    ).astype(jnp.bfloat16)
    row_first = lax.axis_index("tp") * own_rows
    attn_own = lax.psum_scatter(
        jnp.dot(gated, output_projection_weight, preferred_element_type=jnp.float32).astype(
            jnp.bfloat16
        ),
        "tp",
        scatter_dimension=0,
        tiled=True,
    ).astype(jnp.float32)
    stream = (
        lax.dynamic_slice_in_dim(residual, row_first, own_rows, 0).astype(jnp.float32) + attn_own
    )
    normed_own = rms_scaled(stream, feedforward_norm_gain).astype(jnp.bfloat16)
    normed = lax.all_gather(normed_own, ("sp", "tp"), axis=0, tiled=True)
    hid = weights.shape[-1]
    width = weights.shape[0] * weights.shape[2]
    gate_weight = weights[:, 0].reshape(width, hid)
    up_weight = weights[:, 1].reshape(width, hid)
    down_weight = weights[:, 2].reshape(width, hid)
    gate_pre = jnp.dot(normed, gate_weight, preferred_element_type=jnp.float32)
    up_pre = jnp.dot(normed, up_weight, preferred_element_type=jnp.float32)
    hidden = (jax.nn.silu(gate_pre) * up_pre).astype(jnp.bfloat16)
    terms = lax.dot_general(
        hidden, down_weight, (((1,), (1,)), ((), ())), preferred_element_type=jnp.float32
    )
    ffn_own = lax.psum_scatter(
        terms.astype(jnp.bfloat16), ("sp", "tp"), scatter_dimension=0, tiled=True
    ).astype(jnp.float32)
    return (stream + 0.5 * ffn_own).astype(jnp.bfloat16)


def solution(mesh):
    in_specs = (
        P("sp", None),
        P("sp", "tp"),
        P("sp", "tp"),
        P("sp", "tp"),
        P("sp", "tp"),
        P("tp", "sp"),
        P("tp", "sp"),
        P("tp", "sp"),
        P("tp"),
        P("tp", None),
        P(),
        P("sp", "tp"),
        P("sp", "tp"),
        P("sp", "tp"),
    )
    out_specs = P(("sp", "tp"), None)
    return jax.shard_map(
        per_device, mesh=mesh, in_specs=in_specs, out_specs=out_specs, check_vma=False
    )
```

```python
import jax
import jax.numpy as jnp
from jax import lax
from jax.sharding import PartitionSpec as P

QK_DIM = 64
V_DIM = 128
BLOCK = 64


def entering(part, axis, combine, identity):
    place = lax.axis_index(axis)
    gathered = jax.tree.map(lambda a: lax.all_gather(a, axis), part)
    state = jax.tree.map(lambda a, e: jnp.zeros_like(a) + jnp.asarray(e, a.dtype), part, identity)

    def one(step, state):
        return combine(
            state, jax.tree.map(lambda a: lax.dynamic_index_in_dim(a, step, 0, False), gathered)
        )

    return lax.fori_loop(0, place, one, state)


def run_blocks(
    query_h, key_h, value_h, gate_in, forget_logarithm, state_init, norm_init, peak_init
):
    span_len = BLOCK
    blocks_count = query_h.shape[0] // span_len
    query_b = query_h.reshape(blocks_count, span_len, query_h.shape[1])
    key_b = key_h.reshape(blocks_count, span_len, key_h.shape[1])
    value_b = value_h.reshape(blocks_count, span_len, value_h.shape[1])
    gate_b = gate_in.reshape(blocks_count, span_len)
    cum_local = jnp.cumsum(forget_logarithm.reshape(blocks_count, span_len), axis=1)
    cum_last = cum_local[:, -1]
    log_end = cum_last[:, None] - cum_local + gate_b

    def advance(carry, inputs):
        state_now, norm_now, peak_now = carry
        key_blk, value_blk, log_blk, last_blk = inputs
        peak_next = jnp.maximum(last_blk + peak_now, jnp.max(log_blk))
        decay_now = jnp.exp(last_blk + peak_now - peak_next)
        weights = jnp.exp(log_blk - peak_next)
        state_next = decay_now * state_now + jnp.einsum(
            "l,lv,lk->vk", weights, value_blk, key_blk, precision=lax.Precision.HIGHEST
        )
        norm_next = decay_now * norm_now + jnp.einsum(
            "l,lk->k", weights, key_blk, precision=lax.Precision.HIGHEST
        )
        return ((state_next, norm_next, peak_next), (state_now, norm_now, peak_now))

    carried, (state_prev, norm_prev, peak_prev) = lax.scan(
        advance, (state_init, norm_init, peak_init), (key_b, value_b, log_end, cum_last)
    )
    causal = jnp.tril(jnp.ones((span_len, span_len), dtype=bool))
    log_pair = cum_local[:, :, None] - cum_local[:, None, :] + gate_b[:, None, :]
    log_pair = jnp.where(causal[None], log_pair, -jnp.inf)
    inter_log = cum_local + peak_prev[:, None]
    peak_row = jnp.maximum(inter_log, jnp.max(log_pair, axis=2))
    scores = jnp.einsum("cjk,csk->cjs", query_b, key_b, precision=lax.Precision.HIGHEST) * jnp.exp(
        log_pair - peak_row[:, :, None]
    )
    inter_scale = jnp.exp(inter_log - peak_row)
    numer = jnp.einsum("cjs,csv->cjv", scores, value_b, precision=lax.Precision.HIGHEST)
    numer = numer + inter_scale[:, :, None] * jnp.einsum(
        "cjk,cvk->cjv", query_b, state_prev, precision=lax.Precision.HIGHEST
    )
    denominator = jnp.sum(scores, axis=2) + inter_scale * jnp.einsum(
        "cjk,ck->cj", query_b, norm_prev, precision=lax.Precision.HIGHEST
    )
    cell_out = numer / jnp.maximum(jnp.abs(denominator), jnp.exp(-peak_row))[:, :, None]
    return cell_out.reshape(query_h.shape[0], value_h.shape[1])


def by_heads(rows, heads_count):
    tok_count = rows.shape[0]
    return (
        rows.astype(jnp.float32)
        .reshape(tok_count, heads_count, rows.shape[1] // heads_count)
        .transpose(1, 0, 2)
    )


def rms_scaled(values_f32, gain):
    mean_square = jnp.mean(values_f32 * values_f32, axis=-1, keepdims=True)
    return values_f32 * lax.rsqrt(mean_square + 1e-06) * gain.astype(jnp.float32)


def joined(earlier, later):
    total_e, state_e, norm_e, peak_e = earlier
    total_l, state_l, norm_l, peak_l = later
    peak_both = jnp.maximum(total_l + peak_e, peak_l)
    weight_e = jnp.exp(total_l + peak_e - peak_both)
    weight_l = jnp.exp(peak_l - peak_both)
    state_both = weight_e[:, None, None] * state_e + weight_l[:, None, None] * state_l
    norm_both = weight_e[:, None] * norm_e + weight_l[:, None] * norm_l
    return (total_e + total_l, state_both, norm_both, peak_both)


class Fan:
    def __init__(self):
        sp, tp = lax.axis_size("sp"), lax.axis_size("tp")
        self.nz = next(n for n in range(1, sp + 1) if sp % n == 0 and n * n >= sp)
        self.nx = sp // self.nz
        self.cores = 2 if tp % 2 == 0 else 1
        self.ny = tp // self.cores
        place = lax.axis_index("sp")
        self.z, self.x = place // self.nx, lax.rem(place, self.nx)

    def shift_z(self, a, d):
        if d == 0:
            return a
        nz, nx = self.nz, self.nx
        pairs = [(z * nx + x, (z + d) % nz * nx + x) for z in range(nz) for x in range(nx)]
        return lax.ppermute(a, "sp", pairs)

    def shift_x(self, a, e):
        if e == 0:
            return a
        nz, nx = self.nz, self.nx
        pairs = [(z * nx + x, z * nx + (x + e) % nx) for z in range(nz) for x in range(nx)]
        return lax.ppermute(a, "sp", pairs)

    def shift_y(self, a, s):
        if s == 0:
            return a
        ny, nc = self.ny, self.cores
        pairs = [(y * nc + c, (y + s) % ny * nc + c) for y in range(ny) for c in range(nc)]
        return lax.ppermute(a, "tp", pairs)

    def shift_core(self, a, c):
        if c == 0:
            return a
        nc = self.cores
        pairs = [(p, p // nc * nc + (p + c) % nc) for p in range(self.ny * nc)]
        return lax.ppermute(a, "tp", pairs)

    def sp_order(self, z):
        nz, nx = self.nz, self.nx
        return [
            lax.rem(z - d + 2 * nz, nz) * nx + lax.rem(self.x - e + nx, nx)
            for d in range(nz)
            for e in range(nx)
        ]

    def sp_places(self, z):
        nz, nx = self.nz, self.nx
        return [
            lax.rem(z - k + 2 * nz, nz) * nx + lax.rem(self.x - j + nx, nx)
            for k in range(nz)
            for j in range(nx)
        ]

    def tp_order(self):
        place = lax.axis_index("tp")
        y, core = place // self.cores, lax.rem(place, self.cores)
        return [
            lax.rem(y - s + self.ny, self.ny) * self.cores
            + lax.rem(core - c + self.cores, self.cores)
            for c in range(self.cores)
            for s in range(self.ny)
        ]

    def gather_tp(self, block):
        column = jnp.concatenate([self.shift_y(block, s) for s in range(self.ny)])
        return jnp.concatenate([self.shift_core(column, c) for c in range(self.cores)])

    def reduce_tp(self, parts):
        parts = parts.reshape(self.cores, self.ny, -1, parts.shape[1])
        column = parts[0].astype(jnp.float32)
        for c in range(1, self.cores):
            column = column + self.shift_core(parts[c], -c).astype(jnp.float32)
        total = column[0]
        for s in range(1, self.ny):
            total = total + self.shift_y(column[s].astype(jnp.bfloat16), -s).astype(jnp.float32)
        return total


def exchanged(gate, up, down):
    fan = Fan()
    hid = gate.shape[1] // fan.nz
    chunks = jnp.stack(
        [
            jnp.concatenate([w[:, p * hid : (p + 1) * hid] for w in (gate, up, down)], axis=1)
            for p in range(fan.nz)
        ]
    )
    blocks = []
    for d in range(fan.nz):
        chunk = lax.dynamic_index_in_dim(chunks, lax.rem(fan.z + d, fan.nz), 0, False)
        with jax.named_scope(f"weight{d}"):
            block = fan.shift_z(chunk, d)
            blocks += [fan.shift_x(block, e) for e in range(fan.nx)]
    return jnp.concatenate(blocks)


def per_device(
    residual,
    queries,
    projected_key_rows,
    projected_value_rows,
    output_gate_logits,
    input_gate_logits,
    forget_gate_logits,
    extra_forget_logits,
    head_norm_gain,
    output_projection_weight,
    feedforward_norm_gain,
    feedforward_gate_weight,
    up_projection_weight,
    down_projection_weight,
):
    weights = exchanged(
        feedforward_gate_weight, up_projection_weight, down_projection_weight
    )
    tok_here = queries.shape[0]
    heads_here = input_gate_logits.shape[0]
    own_rows = tok_here // lax.axis_size("tp")
    query_h = by_heads(queries, heads_here) * QK_DIM ** (-0.5)
    key_h = by_heads(projected_key_rows, heads_here)
    value_h = by_heads(projected_value_rows, heads_here)
    forget_logarithm = jax.nn.log_sigmoid(forget_gate_logits) + extra_forget_logits
    cum_shard = jnp.cumsum(forget_logarithm, axis=1)
    total_shard = cum_shard[:, -1]
    log_shard = total_shard[:, None] - cum_shard + input_gate_logits
    peak_shard = jnp.max(log_shard, axis=1)
    weight_shard = jnp.exp(log_shard - peak_shard[:, None])
    state_shard = jnp.einsum(
        "hl,hlv,hlk->hvk", weight_shard, value_h, key_h, precision=lax.Precision.HIGHEST
    )
    norm_shard = jnp.einsum("hl,hlk->hk", weight_shard, key_h, precision=lax.Precision.HIGHEST)
    identity = (
        jnp.zeros((heads_here,), jnp.float32),
        jnp.zeros_like(state_shard),
        jnp.zeros_like(norm_shard),
        jnp.full((heads_here,), -1e30, jnp.float32),
    )
    total_before, state_before, norm_before, peak_before = entering(
        (total_shard, state_shard, norm_shard, peak_shard), "sp", joined, identity
    )
    peak_in = jnp.maximum(peak_before, total_before)
    rescale = jnp.exp(peak_before - peak_in)
    state_in = rescale[:, None, None] * state_before
    norm_in = rescale[:, None] * norm_before
    cell_out = jax.vmap(run_blocks)(
        query_h, key_h, value_h, input_gate_logits, forget_logarithm, state_in, norm_in, peak_in
    )
    normed_heads = rms_scaled(cell_out, head_norm_gain.reshape(heads_here, 1, V_DIM))
    gated = (
        normed_heads.transpose(1, 0, 2).reshape(tok_here, heads_here * V_DIM)
        * jax.nn.sigmoid(output_gate_logits.astype(jnp.float32))
    ).astype(jnp.bfloat16)
    fan = Fan()
    row_first = lax.axis_index("tp") * own_rows
    gated = jnp.concatenate(
        [lax.dynamic_slice_in_dim(gated, p * own_rows, own_rows, 0) for p in fan.tp_order()]
    )
    with jax.named_scope("attn"):
        attn_own = fan.reduce_tp(
            jnp.dot(gated, output_projection_weight, preferred_element_type=jnp.float32).astype(
                jnp.bfloat16
            )
        )
    stream = (
        lax.dynamic_slice_in_dim(residual, row_first, own_rows, 0).astype(jnp.float32) + attn_own
    )
    normed_own = rms_scaled(stream, feedforward_norm_gain).astype(jnp.bfloat16)
    hid = weights.shape[1] // 3
    width = feedforward_gate_weight.shape[0]
    ffn_own = jnp.zeros(stream.shape, jnp.float32)
    gathered = []
    for d in range(fan.nz):
        order = fan.sp_order(fan.z + d)
        block = jnp.concatenate(
            [lax.dynamic_slice_in_dim(normed_own, p * width, width, 1) for p in order], axis=1
        )
        with jax.named_scope(f"spread{d}"):
            gathered.append(fan.gather_tp(fan.shift_z(block, d)))
    for d in range(fan.nz):
        pre = jnp.dot(gathered[d], weights[:, : 2 * hid], preferred_element_type=jnp.float32)
        hidden = (jax.nn.silu(pre[:, :hid]) * pre[:, hid:]).astype(jnp.bfloat16)
        terms = lax.dot_general(
            hidden,
            weights[:, 2 * hid :],
            (((1,), (1,)), ((), ())),
            preferred_element_type=jnp.float32,
        ).astype(jnp.bfloat16)
        with jax.named_scope(f"back{d}"):
            part = fan.shift_z(fan.reduce_tp(terms).astype(jnp.bfloat16), -d)
        part = jnp.concatenate(
            [
                lax.dynamic_slice_in_dim(part, p * width, width, 1)
                for p in fan.sp_places(fan.z + d)
            ],
            axis=1,
        )
        ffn_own = ffn_own + part.astype(jnp.float32)
    return (stream + 0.5 * ffn_own).astype(jnp.bfloat16)


def solution(mesh):
    in_specs = (
        P("sp", None),
        P("sp", "tp"),
        P("sp", "tp"),
        P("sp", "tp"),
        P("sp", "tp"),
        P("tp", "sp"),
        P("tp", "sp"),
        P("tp", "sp"),
        P("tp"),
        P("tp", None),
        P(),
        P("sp", "tp"),
        P("sp", "tp"),
        P("sp", "tp"),
    )
    out_specs = P(("sp", "tp"), None)
    return jax.shard_map(
        per_device, mesh=mesh, in_specs=in_specs, out_specs=out_specs, check_vma=False
    )
```

```python
import jax
import jax.numpy as jnp
from jax import lax
from jax.sharding import PartitionSpec as P

QK_DIM = 64
V_DIM = 128
BLOCK = 64


def entering(part, axis, combine, identity):
    place = lax.axis_index(axis)
    gathered = jax.tree.map(lambda a: lax.all_gather(a, axis), part)
    state = jax.tree.map(lambda a, e: jnp.zeros_like(a) + jnp.asarray(e, a.dtype), part, identity)

    def one(step, state):
        return combine(
            state, jax.tree.map(lambda a: lax.dynamic_index_in_dim(a, step, 0, False), gathered)
        )

    return lax.fori_loop(0, place, one, state)


def run_blocks(
    query_h, key_h, value_h, gate_in, forget_logarithm, state_init, norm_init, peak_init
):
    span_len = BLOCK
    blocks_count = query_h.shape[0] // span_len
    query_b = query_h.reshape(blocks_count, span_len, query_h.shape[1])
    key_b = key_h.reshape(blocks_count, span_len, key_h.shape[1])
    value_b = value_h.reshape(blocks_count, span_len, value_h.shape[1])
    gate_b = gate_in.reshape(blocks_count, span_len)
    cum_local = jnp.cumsum(forget_logarithm.reshape(blocks_count, span_len), axis=1)
    cum_last = cum_local[:, -1]
    log_end = cum_last[:, None] - cum_local + gate_b

    def advance(carry, inputs):
        state_now, norm_now, peak_now = carry
        key_blk, value_blk, log_blk, last_blk = inputs
        peak_next = jnp.maximum(last_blk + peak_now, jnp.max(log_blk))
        decay_now = jnp.exp(last_blk + peak_now - peak_next)
        weights = jnp.exp(log_blk - peak_next)
        state_next = decay_now * state_now + jnp.einsum(
            "l,lv,lk->vk", weights, value_blk, key_blk, precision=lax.Precision.HIGHEST
        )
        norm_next = decay_now * norm_now + jnp.einsum(
            "l,lk->k", weights, key_blk, precision=lax.Precision.HIGHEST
        )
        return ((state_next, norm_next, peak_next), (state_now, norm_now, peak_now))

    carried, (state_prev, norm_prev, peak_prev) = lax.scan(
        advance, (state_init, norm_init, peak_init), (key_b, value_b, log_end, cum_last)
    )
    causal = jnp.tril(jnp.ones((span_len, span_len), dtype=bool))
    log_pair = cum_local[:, :, None] - cum_local[:, None, :] + gate_b[:, None, :]
    log_pair = jnp.where(causal[None], log_pair, -jnp.inf)
    inter_log = cum_local + peak_prev[:, None]
    peak_row = jnp.maximum(inter_log, jnp.max(log_pair, axis=2))
    scores = jnp.einsum("cjk,csk->cjs", query_b, key_b, precision=lax.Precision.HIGHEST) * jnp.exp(
        log_pair - peak_row[:, :, None]
    )
    inter_scale = jnp.exp(inter_log - peak_row)
    numer = jnp.einsum("cjs,csv->cjv", scores, value_b, precision=lax.Precision.HIGHEST)
    numer = numer + inter_scale[:, :, None] * jnp.einsum(
        "cjk,cvk->cjv", query_b, state_prev, precision=lax.Precision.HIGHEST
    )
    denominator = jnp.sum(scores, axis=2) + inter_scale * jnp.einsum(
        "cjk,ck->cj", query_b, norm_prev, precision=lax.Precision.HIGHEST
    )
    cell_out = numer / jnp.maximum(jnp.abs(denominator), jnp.exp(-peak_row))[:, :, None]
    return cell_out.reshape(query_h.shape[0], value_h.shape[1])


def by_heads(rows, heads_count):
    tok_count = rows.shape[0]
    return (
        rows.astype(jnp.float32)
        .reshape(tok_count, heads_count, rows.shape[1] // heads_count)
        .transpose(1, 0, 2)
    )


def rms_scaled(values_f32, gain):
    mean_square = jnp.mean(values_f32 * values_f32, axis=-1, keepdims=True)
    return values_f32 * lax.rsqrt(mean_square + 1e-06) * gain.astype(jnp.float32)


def joined(earlier, later):
    total_e, state_e, norm_e, peak_e = earlier
    total_l, state_l, norm_l, peak_l = later
    peak_both = jnp.maximum(total_l + peak_e, peak_l)
    weight_e = jnp.exp(total_l + peak_e - peak_both)
    weight_l = jnp.exp(peak_l - peak_both)
    state_both = weight_e[:, None, None] * state_e + weight_l[:, None, None] * state_l
    norm_both = weight_e[:, None] * norm_e + weight_l[:, None] * norm_l
    return (total_e + total_l, state_both, norm_both, peak_both)


class Fan:
    def __init__(self):
        sp, tp = lax.axis_size("sp"), lax.axis_size("tp")
        self.nz = next(n for n in range(1, sp + 1) if sp % n == 0 and n * n >= sp)
        self.nx = sp // self.nz
        self.cores = 2 if tp % 2 == 0 else 1
        self.ny = tp // self.cores
        place = lax.axis_index("sp")
        self.z, self.x = place // self.nx, lax.rem(place, self.nx)

    def shift_z(self, a, d):
        if d == 0:
            return a
        nz, nx = self.nz, self.nx
        pairs = [(z * nx + x, (z + d) % nz * nx + x) for z in range(nz) for x in range(nx)]
        return lax.ppermute(a, "sp", pairs)

    def shift_x(self, a, e):
        if e == 0:
            return a
        nz, nx = self.nz, self.nx
        pairs = [(z * nx + x, z * nx + (x + e) % nx) for z in range(nz) for x in range(nx)]
        return lax.ppermute(a, "sp", pairs)

    def shift_y(self, a, s):
        if s == 0:
            return a
        ny, nc = self.ny, self.cores
        pairs = [(y * nc + c, (y + s) % ny * nc + c) for y in range(ny) for c in range(nc)]
        return lax.ppermute(a, "tp", pairs)

    def shift_core(self, a, c):
        if c == 0:
            return a
        nc = self.cores
        pairs = [(p, p // nc * nc + (p + c) % nc) for p in range(self.ny * nc)]
        return lax.ppermute(a, "tp", pairs)

    def sp_order(self, z):
        nz, nx = self.nz, self.nx
        return [
            lax.rem(z - d + 2 * nz, nz) * nx + lax.rem(self.x - e + nx, nx)
            for d in range(nz)
            for e in range(nx)
        ]

    def sp_places(self, z):
        nz, nx = self.nz, self.nx
        return [
            lax.rem(z - k + 2 * nz, nz) * nx + lax.rem(self.x - j + nx, nx)
            for k in range(nz)
            for j in range(nx)
        ]

    def tp_order(self):
        place = lax.axis_index("tp")
        y, core = place // self.cores, lax.rem(place, self.cores)
        return [
            lax.rem(y - s + self.ny, self.ny) * self.cores
            + lax.rem(core - c + self.cores, self.cores)
            for c in range(self.cores)
            for s in range(self.ny)
        ]

    def gather_tp(self, block):
        column = jnp.concatenate([self.shift_y(block, s) for s in range(self.ny)])
        return jnp.concatenate([self.shift_core(column, c) for c in range(self.cores)])

    def reduce_tp(self, parts):
        parts = parts.reshape(self.cores, self.ny, -1, parts.shape[1])
        column = parts[0].astype(jnp.float32)
        for c in range(1, self.cores):
            column = column + self.shift_core(parts[c], -c).astype(jnp.float32)
        total = column[0]
        for s in range(1, self.ny):
            total = total + self.shift_y(column[s].astype(jnp.bfloat16), -s).astype(jnp.float32)
        return total


def cut(gate, up, down):
    fan = Fan()
    hid = gate.shape[1] // fan.nz
    return jnp.stack(
        [
            jnp.concatenate([w[:, p * hid : (p + 1) * hid] for w in (gate, up, down)], axis=1)
            for p in range(fan.nz)
        ]
    )


def exchanged(chunks):
    fan = Fan()
    blocks = []
    for d in range(fan.nz):
        chunk = lax.dynamic_index_in_dim(chunks, lax.rem(fan.z + d, fan.nz), 0, False)
        with jax.named_scope(f"weight{d}"):
            block = fan.shift_z(chunk, d)
            blocks += [fan.shift_x(block, e) for e in range(fan.nx)]
    return jnp.concatenate(blocks)


def per_device(
    residual,
    queries,
    projected_key_rows,
    projected_value_rows,
    output_gate_logits,
    input_gate_logits,
    forget_gate_logits,
    extra_forget_logits,
    head_norm_gain,
    output_projection_weight,
    feedforward_norm_gain,
    feedforward_gate_weight,
    up_projection_weight,
    down_projection_weight,
):
    chunks = cut(feedforward_gate_weight, up_projection_weight, down_projection_weight)
    tok_here = queries.shape[0]
    heads_here = input_gate_logits.shape[0]
    own_rows = tok_here // lax.axis_size("tp")
    query_h = by_heads(queries, heads_here) * QK_DIM ** (-0.5)
    key_h = by_heads(projected_key_rows, heads_here)
    value_h = by_heads(projected_value_rows, heads_here)
    forget_logarithm = jax.nn.log_sigmoid(forget_gate_logits) + extra_forget_logits
    cum_shard = jnp.cumsum(forget_logarithm, axis=1)
    total_shard = cum_shard[:, -1]
    log_shard = total_shard[:, None] - cum_shard + input_gate_logits
    peak_shard = jnp.max(log_shard, axis=1)
    weight_shard = jnp.exp(log_shard - peak_shard[:, None])
    state_shard = jnp.einsum(
        "hl,hlv,hlk->hvk", weight_shard, value_h, key_h, precision=lax.Precision.HIGHEST
    )
    norm_shard = jnp.einsum("hl,hlk->hk", weight_shard, key_h, precision=lax.Precision.HIGHEST)
    identity = (
        jnp.zeros((heads_here,), jnp.float32),
        jnp.zeros_like(state_shard),
        jnp.zeros_like(norm_shard),
        jnp.full((heads_here,), -1e30, jnp.float32),
    )
    total_before, state_before, norm_before, peak_before = entering(
        (total_shard, state_shard, norm_shard, peak_shard), "sp", joined, identity
    )
    before = (total_before, state_before, norm_before, peak_before)
    before, chunks = lax.optimization_barrier((before, chunks))
    total_before, state_before, norm_before, peak_before = before
    weights = exchanged(chunks)
    peak_in = jnp.maximum(peak_before, total_before)
    rescale = jnp.exp(peak_before - peak_in)
    state_in = rescale[:, None, None] * state_before
    norm_in = rescale[:, None] * norm_before
    cell_out = jax.vmap(run_blocks)(
        query_h, key_h, value_h, input_gate_logits, forget_logarithm, state_in, norm_in, peak_in
    )
    normed_heads = rms_scaled(cell_out, head_norm_gain.reshape(heads_here, 1, V_DIM))
    gated = (
        normed_heads.transpose(1, 0, 2).reshape(tok_here, heads_here * V_DIM)
        * jax.nn.sigmoid(output_gate_logits.astype(jnp.float32))
    ).astype(jnp.bfloat16)
    fan = Fan()
    row_first = lax.axis_index("tp") * own_rows
    gated = jnp.concatenate(
        [lax.dynamic_slice_in_dim(gated, p * own_rows, own_rows, 0) for p in fan.tp_order()]
    )
    with jax.named_scope("attn"):
        attn_own = fan.reduce_tp(
            jnp.dot(gated, output_projection_weight, preferred_element_type=jnp.float32).astype(
                jnp.bfloat16
            )
        )
    stream = (
        lax.dynamic_slice_in_dim(residual, row_first, own_rows, 0).astype(jnp.float32) + attn_own
    )
    normed_own = rms_scaled(stream, feedforward_norm_gain).astype(jnp.bfloat16)
    hid = weights.shape[1] // 3
    width = feedforward_gate_weight.shape[0]
    ffn_own = jnp.zeros(stream.shape, jnp.float32)
    gathered = []
    for d in range(fan.nz):
        order = fan.sp_order(fan.z + d)
        block = jnp.concatenate(
            [lax.dynamic_slice_in_dim(normed_own, p * width, width, 1) for p in order], axis=1
        )
        with jax.named_scope(f"spread{d}"):
            gathered.append(fan.gather_tp(fan.shift_z(block, d)))
    for d in range(fan.nz):
        pre = jnp.dot(gathered[d], weights[:, : 2 * hid], preferred_element_type=jnp.float32)
        hidden = (jax.nn.silu(pre[:, :hid]) * pre[:, hid:]).astype(jnp.bfloat16)
        terms = lax.dot_general(
            hidden,
            weights[:, 2 * hid :],
            (((1,), (1,)), ((), ())),
            preferred_element_type=jnp.float32,
        ).astype(jnp.bfloat16)
        with jax.named_scope(f"back{d}"):
            part = fan.shift_z(fan.reduce_tp(terms).astype(jnp.bfloat16), -d)
        part = jnp.concatenate(
            [
                lax.dynamic_slice_in_dim(part, p * width, width, 1)
                for p in fan.sp_places(fan.z + d)
            ],
            axis=1,
        )
        ffn_own = ffn_own + part.astype(jnp.float32)
    return (stream + 0.5 * ffn_own).astype(jnp.bfloat16)


def solution(mesh):
    in_specs = (
        P("sp", None),
        P("sp", "tp"),
        P("sp", "tp"),
        P("sp", "tp"),
        P("sp", "tp"),
        P("tp", "sp"),
        P("tp", "sp"),
        P("tp", "sp"),
        P("tp"),
        P("tp", None),
        P(),
        P("sp", "tp"),
        P("sp", "tp"),
        P("sp", "tp"),
    )
    out_specs = P(("sp", "tp"), None)
    return jax.shard_map(
        per_device, mesh=mesh, in_specs=in_specs, out_specs=out_specs, check_vma=False
    )
```
